32 devices in a mesh: rep: 2 (over x), fs: 8 (over z, y), tp: 2 (over core).
Axes of the slice: x: 2, y: 2, z: 4, core: 2. Of those that a mesh axis runs over, the one named last changes fastest.
Arguments:
- tokens: bfloat16 [4096, 2048], P(('rep', 'fs')), may hold values from -6 to 6
- ffn_gate: bfloat16 [2048, 5632], P('fs', 'tp'), may hold values from -0.125 to 0.125
- ffn_up: bfloat16 [2048, 5632], P('fs', 'tp'), may hold values from -0.125 to 0.125
- ffn_down: bfloat16 [5632, 2048], P('tp', 'fs'), may hold values from -0.3125 to 0.3125
- query_proj: bfloat16 [2048, 512], P('fs', 'tp'), may hold values from -0.125 to 0.125
- key_proj: bfloat16 [2048, 512], P('fs', 'tp'), may hold values from -0.125 to 0.125
- value_proj: bfloat16 [2048, 1024], P('fs', 'tp'), may hold values from -0.125 to 0.125
- outgate_proj: bfloat16 [2048, 1024], P('fs', 'tp'), may hold values from -0.125 to 0.125
- output_proj: bfloat16 [1024, 2048], P('tp', 'fs'), may hold values from -0.375 to 0.375
- rank_down: bfloat16 [2048, 16], replicated, may hold values from -0.1875 to 0.1875
- rank_up: bfloat16 [16, 512], replicated, may hold values from -3 to 3
- decay_bias: float32 [512], replicated, may hold values from -0.5 to 8
- head_gain: float32 [1024], replicated, may hold values from 0.1 to 1.9
- norm_gain: float32 [3, 2048], replicated, may hold values from 0.1 to 1.9
- norm_bias: float32 [3, 2048], replicated, may hold values from -2 to 2
Outputs:
- layer_out: bfloat16 [4096, 2048], P(('rep', 'fs'))
The draws below stay inside these ranges and needn't reach their ends.
All inputs are finite; a program needn't handle non-finite values.
Results may differ from the reference program's by a relative error of at most 0.024.
Values may be sent and summed in bfloat16 or wider, within the bound.
A program may use at most 128 MiB of HBM per device.

```python
import jax
import jax.numpy as jnp
from jax import lax

D = 2048
FF = 5632
HEADS = 8
DK = 64
DV = 128
RANK = 16
BLOCK = 64
TOK = 256
TOKENS = 4096
N_TP = 2


def draw_decay_bias(key, part):
    pick_key, slow_key, fast_key, jitter_key = jax.random.split(jax.random.fold_in(key, 11), 4)
    chance = 0.5
    slow_heads = jax.random.uniform(pick_key, (HEADS, 1), jnp.float32) < chance
    slow_level = jax.random.uniform(slow_key, (HEADS, 1), jnp.float32, 5.5, 7.5)
    fast_level = jax.random.uniform(fast_key, (HEADS, 1), jnp.float32, 0.0, 1.5)
    jitter = jax.random.uniform(jitter_key, (HEADS, DK), jnp.float32, -0.5, 0.5)
    return (jnp.where(slow_heads, slow_level, fast_level) + jitter).reshape(HEADS * DK).astype(jnp.float32)


def level_of(own_key, extent, shards, least, largest):
    factor_of, own = 1.0, jax.random.fold_in(own_key, 6)
    for axis_at, shards_of in shards:
        heights = jnp.exp(jax.random.uniform(jax.random.fold_in(own, axis_at), (shards_of,), jnp.float32, least / len(shards), largest / len(shards)))
        factor_of = factor_of * jnp.repeat(heights, extent[axis_at] // shards_of).reshape([-1 if axis == axis_at else 1 for axis in range(len(extent))])
    return factor_of


def bell_draw(key, extent, scale, bound, cuts=(), dtype=jnp.bfloat16):
    result = jax.random.normal(key, extent, jnp.float32) * scale
    if len(cuts) > 0:
        result = level_of(key, extent, cuts, -0.22, 0.18) * result
    return jnp.clip(result, min=-bound, max=bound).astype(dtype)


def setup_inputs(seed: int = 0) -> dict:
    splits = jax.random.split(jax.random.key(seed), 16)
    return {
        "tokens": bell_draw(splits[0], (TOKENS, D), 1.0, 6.0, ((0, 16),)),
        "ffn_gate": bell_draw(splits[1], (D, FF), D ** -0.5, 0.125, ((0, 8), (1, 2))),
        "ffn_up": bell_draw(splits[2], (D, FF), D ** -0.5, 0.125, ((0, 8), (1, 2))),
        "ffn_down": bell_draw(splits[3], (FF, D), (FF // 16) ** -0.5, 0.3125, ((0, 2), (1, 8))),
        "query_proj": bell_draw(splits[4], (D, HEADS * DK), D ** -0.5, 0.125, ((0, 8), (1, 2))),
        "key_proj": bell_draw(splits[5], (D, HEADS * DK), D ** -0.5, 0.125, ((0, 8), (1, 2))),
        "value_proj": bell_draw(splits[6], (D, HEADS * DV), D ** -0.5, 0.125, ((0, 8), (1, 2))),
        "outgate_proj": bell_draw(splits[7], (D, HEADS * DV), D ** -0.5, 0.125, ((0, 8), (1, 2))),
        "output_proj": bell_draw(splits[8], (HEADS * DV, D), (HEADS * DV // 4) ** -0.5, 0.375, ((0, 2), (1, 8))),
        "rank_down": bell_draw(splits[9], (D, RANK), (D // 2) ** -0.5, 0.1875),
        "rank_up": bell_draw(splits[10], (RANK, HEADS * DK), (RANK // 4) ** -0.5, 3.0),
        "decay_bias": draw_decay_bias(jax.random.fold_in(splits[15], 71), 0),
        "head_gain": jnp.clip(1.0 + 0.18 * jax.random.normal(splits[12], (HEADS * DV,), jnp.float32), 0.1, 1.9),
        "norm_gain": jnp.clip(1.0 + 0.18 * jax.random.normal(splits[13], (3, D), jnp.float32), 0.1, 1.9),
        "norm_bias": bell_draw(splits[14], (3, D), 0.3, 2.0, (), jnp.float32),
    }


EPSILON = 1e-05
HEAD_FLOOR = 1.0
RESIDUAL_SCALE = 2.0 ** 0.5
GATE_SOFTNESS = 16.0
FULL_ACCURACY = lax.Precision.HIGHEST

def layer_norm(summed, norm_gain, norm_shift):
    centred = summed - lax.optimization_barrier(jnp.mean(summed, -1, keepdims=True))
    spread = lax.optimization_barrier(jnp.mean(centred * centred, -1, keepdims=True))
    return (centred * lax.rsqrt(spread + EPSILON) * norm_gain + norm_shift).astype(jnp.bfloat16)

def gla_heads(queries, keys_rows, values, decay_logarithm):
    length, head_count, key_width = queries.shape
    value_width = values.shape[-1]
    block_count = length // BLOCK

    def blocks(array):
        return array.reshape(block_count, BLOCK, head_count, array.shape[-1])
    causal = jnp.tril(jnp.ones((BLOCK, BLOCK), bool))[:, :, None, None]

    def advance(running_state, inputs):
        query_block, key_block, value_block, decay_blk = inputs
        decay_prefix = jnp.cumsum(decay_blk, axis=0)
        spread = decay_prefix[:, None] - decay_prefix[None, :]
        weight = jnp.exp(jnp.where(causal, spread, -jnp.inf))
        scores = jnp.einsum('lshk,lhk,shk->hls', weight, query_block, key_block, precision=FULL_ACCURACY)
        within = jnp.einsum('hls,shv->lhv', scores, value_block, precision=FULL_ACCURACY)
        carried_over = jnp.einsum('zew,ewa->zea', query_block * jnp.exp(decay_prefix), running_state, precision=FULL_ACCURACY)
        block_finish = decay_prefix[-1]
        running_state = jnp.exp(block_finish)[:, :, None] * running_state + jnp.einsum('oct,ocy->cty', key_block * jnp.exp(block_finish[None] - decay_prefix), value_block, precision=FULL_ACCURACY)
        return (running_state, within + carried_over)
    initial = jnp.zeros((head_count, key_width, value_width), jnp.float32)
    _, outputs = lax.scan(advance, initial, (blocks(queries), blocks(keys_rows), blocks(values), blocks(decay_logarithm)))
    return outputs.reshape(length, head_count, value_width)

def block_partials(hidden, weight):
    width = weight.shape[0] // N_TP
    summed = jnp.zeros((hidden.shape[0], weight.shape[1]), jnp.float32)
    for block in range(N_TP):
        product = jnp.dot(hidden[:, block * width:(block + 1) * width], weight[block * width:(block + 1) * width], preferred_element_type=jnp.float32)
        rounded = lax.optimization_barrier(product.astype(jnp.bfloat16))
        summed = summed + rounded.astype(jnp.float32)
    return summed

def reference(tokens, ffn_gate, ffn_up, ffn_down, query_proj, key_proj, value_proj, outgate_proj, output_proj, rank_down, rank_up, decay_bias, head_gain, norm_gain, norm_bias):

    def channel_mix(normed):
        gate_rows = jnp.dot(normed, ffn_gate, preferred_element_type=jnp.float32)
        up_rows = jnp.dot(normed, ffn_up, preferred_element_type=jnp.float32)
        hidden = (jax.nn.silu(gate_rows) * up_rows).astype(jnp.bfloat16)
        return block_partials(hidden, ffn_down)

    def one_sequence(rows):
        first = layer_norm(RESIDUAL_SCALE * rows.astype(jnp.float32) + 0.5 * channel_mix(rows), norm_gain[0], norm_bias[0])
        queries = jnp.dot(first, query_proj, preferred_element_type=jnp.float32) * DK ** (-0.5)
        keys_rows = jnp.dot(first, key_proj, preferred_element_type=jnp.float32)
        values = jnp.dot(first, value_proj, preferred_element_type=jnp.float32)
        gates = jnp.dot(first, outgate_proj, preferred_element_type=jnp.float32)
        rank_rows = jnp.dot(first, rank_down, preferred_element_type=jnp.float32)
        decay_source = jnp.dot(rank_rows, rank_up.astype(jnp.float32), precision=FULL_ACCURACY) + decay_bias
        decay_logarithm = jax.nn.log_sigmoid(decay_source) / GATE_SOFTNESS
        length = rows.shape[0]
        heads_out = gla_heads(queries.reshape(length, HEADS, DK), keys_rows.reshape(length, HEADS, DK), values.reshape(length, HEADS, DV), decay_logarithm.reshape(length, HEADS, DK))
        scaled = heads_out * lax.rsqrt(lax.optimization_barrier(jnp.mean(heads_out * heads_out, -1, keepdims=True)) + HEAD_FLOOR)
        scaled = scaled * head_gain.reshape(HEADS, DV)
        mixed = (scaled.reshape(length, HEADS * DV) * jax.nn.silu(gates)).astype(jnp.bfloat16)
        second = layer_norm(RESIDUAL_SCALE * first.astype(jnp.float32) + block_partials(mixed, output_proj), norm_gain[1], norm_bias[1])
        return layer_norm(RESIDUAL_SCALE * second.astype(jnp.float32) + 0.5 * channel_mix(second), norm_gain[2], norm_bias[2])
    sequences = tokens.reshape(TOKENS // TOK, TOK, D)
    return lax.map(one_sequence, sequences).reshape(TOKENS, D)
```

```python
import functools

import jax
import jax.numpy as jnp
from jax import lax
from jax.experimental import pallas as pl
from jax.experimental.pallas import tpu as pltpu
from jax.sharding import PartitionSpec as P

DK = 64
DV = 128
CHUNK = 16

EPSILON = 1e-05
HEAD_FLOOR = 1.0
RESIDUAL_SCALE = 2.0**0.5
GATE_SOFTNESS = 16.0
FULL_ACCURACY = lax.Precision.HIGHEST
MESH = pl.DeviceIdType.MESH
HBM = pl.BlockSpec(memory_space=pltpu.MemorySpace.HBM)
VMEM = pl.BlockSpec(memory_space=pltpu.MemorySpace.VMEM)


def gather_kernel(nz, ny, count, *refs):
    ins, outs = refs[:count], refs[count : 2 * count]
    send_main, recv_main, send_far, recv_far, local_sem = refs[2 * count :]
    rep = lax.axis_index("rep")
    fs = lax.axis_index("fs")
    z, y = fs // ny, fs % ny

    def place(dz, dy):
        return lax.rem(z + nz - dz, nz) * ny + lax.rem(y + ny - dy, ny)

    def peer(dz, dy):
        return lax.rem(z + dz, nz) * ny + lax.rem(y + dy, ny)

    partners = [{"fs": peer(dz, 0)} for dz in range(1, nz)]
    partners += [{"fs": peer(0, dy)} for dy in range(1, ny)]
    partners += [{"rep": 1 - rep}]
    barrier = pltpu.get_barrier_semaphore()
    for partner in partners:
        pl.semaphore_signal(barrier, inc=1, device_id=partner, device_id_type=MESH)
    pl.semaphore_wait(barrier, len(partners))

    def main_rows(at):
        rows = ins[at].shape[0]
        return pl.ds(pl.multiple_of(rep * (rows * 3 // 8), 8), rows * 5 // 8)

    def main_copy(at, dz, dy):
        rows = main_rows(at)
        over_y = dy > 0
        block = place(dz, 0) if over_y else fs
        source = outs[at].at[block, rows] if over_y and dz > 0 else ins[at].at[rows]
        return pltpu.make_async_remote_copy(
            src_ref=source,
            dst_ref=outs[at].at[block, rows],
            send_sem=send_main.at[at, dz, dy],
            recv_sem=recv_main.at[at, dz, dy],
            device_id={"fs": peer(0, dy) if over_y else peer(dz, 0)},
            device_id_type=MESH,
        )

    def main_landed(at, dz, dy):
        rows = main_rows(at)
        landed = outs[at].at[place(dz, dy), rows]
        return pltpu.make_async_remote_copy(
            src_ref=landed,
            dst_ref=landed,
            send_sem=send_main.at[at, dz, dy],
            recv_sem=recv_main.at[at, dz, dy],
            device_id={"fs": peer(dz, 0) if dy == 0 else peer(0, dy)},
            device_id_type=MESH,
        )

    def far_copy(at, dz, dy, rows):
        moved = outs[at].at[place(dz, dy), rows]
        return pltpu.make_async_remote_copy(
            src_ref=moved,
            dst_ref=moved,
            send_sem=send_far.at[at, dz, dy],
            recv_sem=recv_far.at[at, dz, dy],
            device_id={"rep": 1 - rep},
            device_id_type=MESH,
        )

    def own_far_rows(at):
        rows = ins[at].shape[0]
        return pl.ds(pl.multiple_of(rep * (rows * 5 // 8), 8), rows * 3 // 8)

    def other_far_rows(at):
        rows = ins[at].shape[0]
        return pl.ds(pl.multiple_of((1 - rep) * (rows * 5 // 8), 8), rows * 3 // 8)

    started = []
    locals_ = []
    for at in range(count):
        for dz in range(1, nz):
            copy = main_copy(at, dz, 0)
            copy.start()
            started.append(copy)
        for dy in range(1, ny):
            copy = main_copy(at, 0, dy)
            copy.start()
            started.append(copy)
        copy = pltpu.make_async_copy(ins[at], outs[at].at[fs], local_sem.at[at])
        copy.start()
        locals_.append(copy)

    def after_z(at):
        for dz in range(1, nz):
            main_landed(at, dz, 0).wait_recv()
            for dy in range(1, ny):
                copy = main_copy(at, dz, dy)
                copy.start()
                started.append(copy)
            copy = far_copy(at, dz, 0, own_far_rows(at))
            copy.start()
            started.append(copy)

    def after_y(at):
        for dz in range(nz):
            for dy in range(1, ny):
                main_landed(at, dz, dy).wait_recv()
                copy = far_copy(at, dz, dy, own_far_rows(at))
                copy.start()
                started.append(copy)

    for at in range(count + 1):
        if at < count:
            after_z(at)
        if at > 0:
            after_y(at - 1)
    for at in range(count):
        for dz in range(nz):
            for dy in range(ny):
                if dz or dy:
                    far_copy(at, dz, dy, other_far_rows(at)).wait_recv()
    for copy in started:
        copy.wait_send()
    for copy in locals_:
        copy.wait()


def gather_all(mesh_shape, shards):
    n = mesh_shape["fs"]
    ny = 2 ** ((n.bit_length() - 1) // 2)
    nz = n // ny
    count = len(shards)
    semaphores = pltpu.SemaphoreType.DMA((count, nz, ny))
    return pl.pallas_call(
        functools.partial(gather_kernel, nz, ny, count),
        out_shape=[jax.ShapeDtypeStruct((n, *shard.shape), shard.dtype) for shard in shards],
        in_specs=[VMEM] * count,
        out_specs=[HBM] * count,
        scratch_shapes=[semaphores] * 4 + [pltpu.SemaphoreType.DMA((count,))],
        compiler_params=pltpu.CompilerParams(collective_id=0, has_side_effects=True),
        name="gather_weights",
    )(*shards)


def settle_kernel(ntp, factor, part_ref, rest_ref, gain_ref, shift_ref, out_ref, got, send, recv):
    tp = lax.axis_index("tp")
    barrier = pltpu.get_barrier_semaphore()
    for d in range(1, ntp):
        pl.semaphore_signal(
            barrier, inc=1, device_id={"tp": lax.rem(tp + d, ntp)}, device_id_type=MESH
        )
    pl.semaphore_wait(barrier, ntp - 1)
    copies = []
    for d in range(1, ntp):
        copy = pltpu.make_async_remote_copy(
            src_ref=part_ref,
            dst_ref=got.at[d - 1],
            send_sem=send.at[d - 1],
            recv_sem=recv.at[d - 1],
            device_id={"tp": lax.rem(tp + d, ntp)},
            device_id_type=MESH,
        )
        copy.start()
        copies.append(copy)
    for copy in copies:
        copy.wait()
    tile = 16

    def one(step, carry):
        rows = pl.ds(pl.multiple_of(step * tile, tile), tile)
        summed = part_ref[rows, :].astype(jnp.float32)
        for d in range(ntp - 1):
            summed = summed + got[d, rows, :].astype(jnp.float32)
        summed = RESIDUAL_SCALE * rest_ref[rows, :].astype(jnp.float32) + factor * summed
        centred = summed - jnp.mean(summed, -1, keepdims=True)
        spread = jnp.mean(centred * centred, -1, keepdims=True)
        normed = centred * lax.rsqrt(spread + EPSILON) * gain_ref[...] + shift_ref[...]
        out_ref[rows, :] = normed.astype(jnp.bfloat16)
        return carry

    lax.fori_loop(0, part_ref.shape[0] // tile, one, 0)


def settle(ntp, which, partial_value, residual_rows, factor, norm_gain, norm_bias):
    rows, width = partial_value.shape
    return pl.pallas_call(
        functools.partial(settle_kernel, ntp, factor),
        out_shape=jax.ShapeDtypeStruct((rows, width), jnp.bfloat16),
        in_specs=[VMEM] * 4,
        out_specs=VMEM,
        scratch_shapes=[
            pltpu.VMEM((ntp - 1, rows, width), jnp.bfloat16),
            pltpu.SemaphoreType.DMA((ntp - 1,)),
            pltpu.SemaphoreType.DMA((ntp - 1,)),
        ],
        compiler_params=pltpu.CompilerParams(collective_id=1 + which, has_side_effects=True),
        name="settle_" + str(which),
    )(
        partial_value.astype(jnp.bfloat16),
        residual_rows,
        norm_gain[which : which + 1],
        norm_bias[which : which + 1],
    )


def heads_kernel(kc, vc, proj_ref, decay_ref, gain_ref, out_ref, prefix, total, state):
    rows = proj_ref.shape[0]
    c = CHUNK
    t_at = lax.broadcasted_iota(jnp.int32, (rows, rows), 0)
    s_at = lax.broadcasted_iota(jnp.int32, (rows, rows), 1)
    lower = ((t_at >= s_at) & (t_at // c == s_at // c)).astype(jnp.float32)
    prefix[...] = jnp.dot(
        lower, decay_ref[...], precision=FULL_ACCURACY, preferred_element_type=jnp.float32
    )
    same = (
        lax.broadcasted_iota(jnp.int32, (kc, vc), 0) // DK
        == lax.broadcasted_iota(jnp.int32, (kc, vc), 1) // DV
    ).astype(jnp.bfloat16)
    turned = (
        lax.broadcasted_iota(jnp.int32, (vc, kc), 0) // DV
        == lax.broadcasted_iota(jnp.int32, (vc, kc), 1) // DK
    ).astype(jnp.float32)
    spot = lax.rem(lax.broadcasted_iota(jnp.int32, (rows, kc), 0), c)
    scale = DK ** (-0.5)
    total[...] = jnp.zeros_like(total)

    def shifted(d, carry):
        q = proj_ref[:, :kc] * scale
        k = pltpu.roll(proj_ref[:, kc : 2 * kc], d, 0)
        v = pltpu.roll(proj_ref[:, 2 * kc : 2 * kc + vc], d, 0)
        g = prefix[...]
        weight = jnp.exp(jnp.where(spot >= d, g - pltpu.roll(g, d, 0), -jnp.inf))
        score = jnp.dot(
            (q * k * weight).astype(jnp.bfloat16), same, preferred_element_type=jnp.float32
        )
        total[...] += score * v
        return carry

    lax.fori_loop(0, c, shifted, 0)
    state[...] = jnp.zeros_like(state)

    def advance(i, carry):
        at = pl.ds(pl.multiple_of(i * c, c), c)
        g = prefix[at, :]
        q = proj_ref[at, :kc] * scale * jnp.exp(g)
        total[at, :] += lax.dot_general(
            q.astype(jnp.bfloat16),
            state[...].astype(jnp.bfloat16),
            (((1,), (1,)), ((), ())),
            preferred_element_type=jnp.float32,
        )
        end = g[c - 1 : c, :]
        k = proj_ref[at, kc : 2 * kc] * jnp.exp(end - g)
        v = proj_ref[at, 2 * kc : 2 * kc + vc]
        fresh = lax.dot_general(
            v.astype(jnp.bfloat16),
            k.astype(jnp.bfloat16),
            (((0,), (0,)), ((), ())),
            preferred_element_type=jnp.float32,
        )
        state[...] = state[...] * jnp.exp(end) + fresh * turned
        return carry

    lax.fori_loop(0, rows // c, advance, 0)
    for head in range(vc // DV):
        cols = slice(head * DV, (head + 1) * DV)
        out = total[:, cols]
        gate = proj_ref[:, 2 * kc + vc + head * DV : 2 * kc + vc + (head + 1) * DV]
        norm = lax.rsqrt(jnp.mean(out * out, -1, keepdims=True) + HEAD_FLOOR)
        value = out * norm * gain_ref[:, cols] * (gate / (1.0 + jnp.exp(-gate)))
        out_ref[:, cols] = value.astype(jnp.bfloat16)


def heads(kc, vc, projected, decay, gain):
    rows = projected.shape[0]
    return pl.pallas_call(
        functools.partial(heads_kernel, kc, vc),
        out_shape=jax.ShapeDtypeStruct((rows, vc), jnp.bfloat16),
        in_specs=[VMEM] * 3,
        out_specs=VMEM,
        scratch_shapes=[
            pltpu.VMEM((rows, kc), jnp.float32),
            pltpu.VMEM((rows, vc), jnp.float32),
            pltpu.VMEM((vc, kc), jnp.float32),
        ],
        name="gla_heads",
    )(projected, decay, gain)


def across(rows, blocks):
    return jnp.concatenate(
        [
            jnp.dot(rows, blocks[at], preferred_element_type=jnp.float32).astype(jnp.bfloat16)
            for at in range(blocks.shape[0])
        ],
        axis=1,
    )


def channel_mix(normed, gate_full, up_full, down_blocks):
    gate_rows = jnp.dot(normed, gate_full, preferred_element_type=jnp.float32)
    up_rows = jnp.dot(normed, up_full, preferred_element_type=jnp.float32)
    hidden = (jax.nn.silu(gate_rows) * up_rows).astype(jnp.bfloat16)
    return across(hidden, down_blocks)


def per_device(
    mesh_shape,
    tokens,
    ffn_gate,
    ffn_up,
    ffn_down,
    query_proj,
    key_proj,
    value_proj,
    outgate_proj,
    output_proj,
    rank_down,
    rank_up,
    decay_bias,
    head_gain,
    norm_gain,
    norm_bias,
):
    ntp = mesh_shape["tp"]
    key_cols = query_proj.shape[1]
    value_cols = value_proj.shape[1]
    joined = jnp.concatenate([query_proj, key_proj, value_proj, outgate_proj], axis=1)
    gathered = gather_all(mesh_shape, [ffn_gate, ffn_up, ffn_down, joined, output_proj])
    gate_full, up_full, joined_full = (
        gathered[at].reshape(-1, gathered[at].shape[2]) for at in (0, 1, 3)
    )
    down_blocks, output_blocks = gathered[2], gathered[4]

    first = settle(
        ntp,
        0,
        channel_mix(tokens, gate_full, up_full, down_blocks),
        tokens,
        0.5,
        norm_gain,
        norm_bias,
    )
    projected = jnp.dot(first, joined_full, preferred_element_type=jnp.float32)
    position = lax.axis_index("tp")
    rank_rows = jnp.dot(first, rank_down, preferred_element_type=jnp.float32)
    up_block = lax.dynamic_slice_in_dim(rank_up, position * key_cols, key_cols, 1)
    bias_block = lax.dynamic_slice_in_dim(decay_bias, position * key_cols, key_cols, 0)
    decay_source = (
        jnp.dot(rank_rows, up_block.astype(jnp.float32), precision=FULL_ACCURACY) + bias_block
    )
    decay_logarithm = jax.nn.log_sigmoid(decay_source) / GATE_SOFTNESS
    gain_block = lax.dynamic_slice_in_dim(head_gain, position * value_cols, value_cols, 0)
    mixed = heads(key_cols, value_cols, projected, decay_logarithm, gain_block[None])
    second = settle(ntp, 1, across(mixed, output_blocks), first, 1.0, norm_gain, norm_bias)
    return settle(
        ntp,
        2,
        channel_mix(second, gate_full, up_full, down_blocks),
        second,
        0.5,
        norm_gain,
        norm_bias,
    )


def solution(mesh):
    return jax.shard_map(
        functools.partial(per_device, dict(mesh.shape)),
        mesh=mesh,
        in_specs=(
            P(("rep", "fs"), None),
            P("fs", "tp"),
            P("fs", "tp"),
            P("tp", "fs"),
            P("fs", "tp"),
            P("fs", "tp"),
            P("fs", "tp"),
            P("fs", "tp"),
            P("tp", "fs"),
            P(),
            P(),
            P(),
            P(),
            P(),
            P(),
        ),
        out_specs=P(("rep", "fs"), None),
        check_vma=False,
    )
```
